1024 devices in a mesh: rep: 4 (over z_hi), fs: 32 (over z_lo, y), tp: 8 (over x, core).
Axes of the slice: x: 4, y: 4, z: 32 (z_hi: 4, z_lo: 8; z = z_hi * 8 + z_lo), core: 2. Of those that a mesh axis runs over, the one named last changes fastest.
Arguments:
- hidden_pre: bfloat16 [65536, 4096], P(('rep', 'fs'), 'tp'), may hold values from -6 to 6
- out_grad: bfloat16 [65536, 2048], P(('rep', 'fs')), may hold values from -24 to 24
- down_weight: bfloat16 [2048, 4096], P('fs', 'tp'), may hold values from -0.09375 to 0.09375
Outputs:
- hidden_grad: bfloat16 [65536, 4096], P(('rep', 'fs'), 'tp')
- weight_grad: float32 [2048, 4096], P('fs', 'tp')
The draws below stay inside these ranges and needn't reach their ends.
All inputs are finite; a program needn't handle non-finite values.
Results may differ from the reference program's by a relative error of at most 0.0049.
Values may be sent and summed in bfloat16 or wider, within the bound.
A program may use at most 32 MiB of HBM per device.

```python
import jax
import jax.numpy as jnp
from jax import lax

D = 2048
FF = 4096
TOK_DEV = 512
TOKENS = 65536


def strengthened(array, key, source, target, shards_of, factor):
    def block_of(axis_at):
        return (jnp.arange(array.shape[axis_at]) // (array.shape[axis_at] // shards_of)).reshape((-1,) + (1,) * (array.ndim - 1 - axis_at))

    one_side = jax.random.permutation(key, shards_of)[block_of(target)]
    far = (block_of(target) + shards_of // 2) % shards_of
    return jnp.where((block_of(source) == one_side) | (block_of(source) == far), factor * array, array)


def level_of(key, dims, split, low, largest):
    def one(axis_at, parts):
        draws = jax.random.uniform(jax.random.fold_in(jax.random.fold_in(key, 6), axis_at), (parts,), jnp.float32, low / len(split), largest / len(split))
        return jnp.repeat(jnp.exp(draws), dims[axis_at] // parts).reshape((-1,) + (1,) * (len(dims) - axis_at - 1))

    level = one(*split[0])
    for cut in split[1:]:
        level = level * one(*cut)
    return level


def bell_draw(stream_key, shape, deviation, most, split=(), held_as=jnp.bfloat16):
    entries = deviation * jax.random.normal(stream_key, shape, jnp.float32)
    if split:
        entries = entries * level_of(stream_key, shape, split, -0.22, 0.18)
    return jnp.clip(entries, -most, most).astype(held_as)


def gaussian_with(key, dims, scale, limit, shards, heavy, held_as=jnp.bfloat16):
    result = scale * jax.random.normal(key, dims, jnp.float32)
    if shards:
        result = result * level_of(key, dims, shards, -0.22, 0.18)
    return jnp.clip(strengthened(result, jax.random.fold_in(key, 3), *heavy), -limit, limit).astype(held_as)


def setup_inputs(seed: int = 0) -> dict:
    key_list = jax.random.split(jax.random.key(seed), 4)
    hidden_pre = bell_draw(key_list[0], (TOKENS, FF), 1.0, 6.0, ((0, 128), (1, 8)))
    out_grad = gaussian_with(key_list[1], (TOKENS, D), 1.0, 24.0, ((0, 128),), (0, 1, 128, 5.5))
    down_weight = bell_draw(key_list[2], (D, FF), FF ** -0.5, 0.09375, ((0, 32), (1, 8)))
    return dict(hidden_pre=hidden_pre, out_grad=out_grad, down_weight=down_weight)


def reference(hidden_pre, out_grad, down_weight):
    count = TOKENS // TOK_DEV
    pre_blocks = hidden_pre.reshape(count, TOK_DEV, FF)
    grad_blocks = out_grad.reshape(count, TOK_DEV, D)

    def one_block(total, inputs):
        pre_rows, grad_rows = inputs
        positive = jnp.maximum(pre_rows.astype(jnp.float32), jnp.float32(0.0))
        back = jnp.dot(grad_rows, down_weight, preferred_element_type=jnp.float32)
        hidden_rows = (2.0 * positive * back).astype(jnp.bfloat16)
        act = (positive * positive).astype(jnp.bfloat16)
        part = lax.dot_general(grad_rows, act, (((0,), (0,)), ((), ())), preferred_element_type=jnp.float32)
        part = part.astype(jnp.bfloat16)
        return total + part.astype(jnp.float32), hidden_rows

    start = jnp.zeros((D, FF), jnp.float32)
    total, hidden_rows = lax.scan(one_block, start, (pre_blocks, grad_blocks))
    hidden_grad = hidden_rows.reshape(TOKENS, FF)
    weight_grad = total * jnp.float32(TOKENS ** -0.5)
    return hidden_grad, weight_grad
```

```python
import functools
import math

import jax
import jax.numpy as jnp
from jax import lax
from jax.experimental import pallas as pl
from jax.experimental.pallas import tpu as pltpu
from jax.sharding import PartitionSpec as P

MESH = pl.DeviceIdType.MESH
NY = 4
NK = 8
NP = 4
ZOFF = (3, -3, 2, -2, 1, -1)
F32 = jnp.float32
BF16 = jnp.bfloat16


def kernel(
    scale, nrep,
    hp_hbm, og_hbm, w_hbm, hg_ref, wo_ref,
    hp, og, ogt, act, part, arecv, bmerged, brecv, zsend, zrecv, qsend, qrecv, tsend, trecv, wall, back,
    lsem, as_, ar_, us_, ur_, ms_, mr_, zs_, zr_, qs_, qr_, ts_, tr_, gzs, gzr, gys, gyr, near4,
):
    nz = nrep * NK
    h = lax.axis_index("rep")
    f = lax.axis_index("fs")
    k = f // NY
    j = lax.rem(f, NY)
    z = h * NK + k
    rows = w_hbm.shape[0]
    cols = w_hbm.shape[1] // NP
    quarter = rows // nrep
    half = rows // 2
    j1, j2, j3 = lax.rem(j + 1, NY), lax.rem(j + 2, NY), lax.rem(j + 3, NY)

    def ydev(jj):
        return {"fs": k * NY + jj}

    def zdev(d):
        zz = lax.rem(z + d + nz, nz)
        return {"rep": zz // NK, "fs": lax.rem(zz, NK) * NY + j}

    def kk(d):
        return lax.rem(k + d + NK, NK)

    right, left = ydev(j1), ydev(j3)
    sends = []

    def send(src, dst, ss, rs, dev):
        c = pltpu.make_async_remote_copy(
            src_ref=src, dst_ref=dst, send_sem=ss, recv_sem=rs, device_id=dev, device_id_type=MESH
        )
        c.start()
        sends.append(c)

    def got(dst, rs):
        pltpu.make_async_remote_copy(
            src_ref=dst, dst_ref=dst, send_sem=rs, recv_sem=rs, device_id=right, device_id_type=MESH
        ).wait_recv()

    barrier = pltpu.get_barrier_semaphore()
    peers = [right, left] + [zdev(d) for d in (1, -1, 2, -2, 3, -3, 4, -4)]
    for peer in peers:
        pl.semaphore_signal(barrier, inc=1, device_id=peer, device_id_type=MESH)

    wide = NY * rows
    loads = []

    def load(src, dst, i):
        c = pltpu.make_async_copy(src, dst, lsem.at[i])
        c.start()
        loads.append(c)

    load(hp_hbm, hp, 0)
    for i in range(NK):
        load(og_hbm.at[:, pl.ds(i * wide, wide)], og.at[i], 1 + i)
    load(w_hbm, wall.at[k, j], 1 + NK)

    loads[0].wait()
    pos = jnp.maximum(hp[...].astype(F32), 0.0)
    act[...] = (pos * pos).astype(BF16)

    def comp_one(p, i):
        res = jnp.dot(
            ogt[i], act[:, p * cols:(p + 1) * cols], preferred_element_type=F32
        ).astype(BF16)
        for jj in range(NY):
            part[p, jj, i] = res[jj * rows:(jj + 1) * rows]

    def comp(p):
        @pl.loop(0, NK)
        def _(i):
            comp_one(p, i)

    for i in range(NK):
        loads[1 + i].wait()
        ogt[i] = og[i].T
    comp(0)
    loads[1 + NK].wait()
    pl.semaphore_wait(barrier, len(peers))
    for d in (4, -4):
        pl.semaphore_signal(near4.at[0], inc=1, device_id=zdev(d), device_id_type=MESH)

    lo, hi = pl.ds(0, NK // 2), pl.ds(NK // 2, NK // 2)

    def send_a(p):
        send(part.at[p, j2, lo], arecv.at[p, 0], as_.at[p, 0], ar_.at[p, 0], right)
        send(part.at[p, j2, hi], arecv.at[p, 1], as_.at[p, 1], ar_.at[p, 1], left)

    def send_u(p):
        send(part.at[p, j1, hi], brecv.at[p, 0, hi], us_.at[p, 0], ur_.at[p, 0], right)
        send(part.at[p, j3, lo], brecv.at[p, 1, lo], us_.at[p, 1], ur_.at[p, 1], left)

    def merge(p):
        got(arecv.at[p, 0], ar_.at[p, 0])
        bmerged[p, 0] = (part[p, j1, lo].astype(F32) + arecv[p, 0].astype(F32)).astype(BF16)
        send(bmerged.at[p, 0], brecv.at[p, 0, lo], ms_.at[p, 0], mr_.at[p, 0], right)
        got(arecv.at[p, 1], ar_.at[p, 1])
        bmerged[p, 1] = (part[p, j3, hi].astype(F32) + arecv[p, 1].astype(F32)).astype(BF16)
        send(bmerged.at[p, 1], brecv.at[p, 1, hi], ms_.at[p, 1], mr_.at[p, 1], left)

    def ysum(p, i):
        return part[p, j, i].astype(F32) + brecv[p, 0, i].astype(F32) + brecv[p, 1, i].astype(F32)

    def recv_b(p):
        got(brecv.at[p, 0, hi], ur_.at[p, 0])
        got(brecv.at[p, 1, lo], ur_.at[p, 1])
        got(brecv.at[p, 0, lo], mr_.at[p, 0])
        got(brecv.at[p, 1, hi], mr_.at[p, 1])

        @pl.loop(0, NK)
        def _(i):
            zsend[p, i] = ysum(p, i).astype(BF16)

        far = kk(4)
        send(zsend.at[p, far, pl.ds(half, half)], zrecv.at[p, 6, pl.ds(half, half)], zs_.at[p, 6], zr_.at[p, 6], zdev(4))
        send(zsend.at[p, far, pl.ds(0, half)], zrecv.at[p, 6, pl.ds(0, half)], zs_.at[p, 7], zr_.at[p, 7], zdev(-4))
        for s, d in enumerate(ZOFF):
            send(zsend.at[p, kk(d)], zrecv.at[p, s], zs_.at[p, s], zr_.at[p, s], zdev(d))

    def recv_z(p):
        got(zrecv.at[p, 6, pl.ds(half, half)], zr_.at[p, 6])
        got(zrecv.at[p, 6, pl.ds(0, half)], zr_.at[p, 7])
        for s in range(len(ZOFF)):
            got(zrecv.at[p, s], zr_.at[p, s])
        q = ysum(p, k)
        for s in range(len(ZOFF) + 1):
            q = q + zrecv[p, s].astype(F32)
        qsend[p] = q.astype(BF16)
        for r in range(nrep):
            send(
                qsend.at[p, pl.ds(r * quarter, quarter)], qrecv.at[p, h], qs_.at[p, r], qr_.at[p, h],
                {"rep": r, "fs": kk(4) * NY + j},
            )

    def recv_q(p):
        for r in range(nrep):
            got(qrecv.at[p, r], qr_.at[p, r])
        t = qrecv[p, 0].astype(F32)
        for r in range(1, nrep):
            t = t + qrecv[p, r].astype(F32)
        tsend[p] = (t * scale).astype(BF16)
        for r in range(nrep):
            send(tsend.at[p], trecv.at[p, h], ts_.at[p, r], tr_.at[p, h], {"rep": r, "fs": kk(4) * NY + j})

    def recv_t(p):
        for r in range(nrep):
            got(trecv.at[p, r], tr_.at[p, r])
            wo_ref[r * quarter:(r + 1) * quarter, p * cols:(p + 1) * cols] = trecv[p, r].astype(F32)

    def gz(s):
        lower, upper = kk(-s), kk(s)
        if s > 0:
            got(wall.at[lower, j], gzr.at[s - 1, 0])
            got(wall.at[upper, j], gzr.at[s - 1, 1])
        if s < NK // 2 - 1:
            send(wall.at[lower, j], wall.at[lower, j], gzs.at[s, 0], gzr.at[s, 0], zdev(1))
            send(wall.at[upper, j], wall.at[upper, j], gzs.at[s, 1], gzr.at[s, 1], zdev(-1))
        else:
            a = wall.at[lower, j, pl.ds(0, half)]
            b = wall.at[upper, j, pl.ds(half, half)]
            send(a, a, gzs.at[s, 0], gzr.at[s, 0], zdev(1))
            send(b, b, gzs.at[s, 1], gzr.at[s, 1], zdev(-1))

    def gy_own():
        far = kk(4)
        got(wall.at[far, j, pl.ds(0, half)], gzr.at[NK // 2 - 1, 0])
        got(wall.at[far, j, pl.ds(half, half)], gzr.at[NK // 2 - 1, 1])
        a, b = wall.at[lo, j], wall.at[hi, j]
        send(a, a, gys.at[0, 0], gyr.at[0, 0], right)
        send(b, b, gys.at[0, 1], gyr.at[0, 1], left)
        send(b, b, gys.at[1, 0], gyr.at[1, 0], right)
        send(a, a, gys.at[1, 1], gyr.at[1, 1], left)

    def gy_forward():
        a, b = wall.at[lo, j3], wall.at[hi, j1]
        got(a, gyr.at[0, 0])
        send(a, a, gys.at[2, 0], gyr.at[2, 0], right)
        got(b, gyr.at[0, 1])
        send(b, b, gys.at[2, 1], gyr.at[2, 1], left)

    def gy_done():
        got(wall.at[hi, j3], gyr.at[1, 0])
        got(wall.at[lo, j1], gyr.at[1, 1])
        got(wall.at[lo, j2], gyr.at[2, 0])
        got(wall.at[hi, j2], gyr.at[2, 1])

    send_a(0)
    send_u(0)
    gz(0)
    comp(1)
    send_a(1)
    merge(0)
    send_u(1)
    gz(1)
    comp(2)
    send_a(2)
    merge(1)
    send_u(2)
    pl.semaphore_wait(near4.at[0], 2)
    for d in (4, -4):
        pl.semaphore_signal(near4.at[1], inc=1, device_id=zdev(d), device_id_type=MESH)
    recv_b(0)
    gz(2)
    comp(3)
    send_a(3)
    merge(2)
    send_u(3)
    recv_b(1)
    pl.semaphore_wait(near4.at[1], 2)
    recv_z(0)
    gz(3)
    merge(3)
    gy_own()
    recv_b(2)
    recv_z(1)
    recv_q(0)
    recv_b(3)
    recv_z(2)
    recv_q(1)
    recv_z(3)
    recv_q(2)
    gy_forward()
    recv_t(0)
    recv_t(1)
    recv_q(3)
    recv_t(2)
    gy_done()

    back[...] = jnp.zeros_like(back)

    @pl.loop(0, NK)
    def _(i):
        back[...] += jnp.dot(
            og[i], wall[i].reshape(wide, wall.shape[-1]), preferred_element_type=F32
        )

    hg_ref[...] = (2.0 * jnp.maximum(hp[...].astype(F32), 0.0) * back[...]).astype(BF16)
    recv_t(3)
    for c in sends:
        c.wait_send()


def body(hidden_pre, out_grad, down_weight):
    tok, ff = hidden_pre.shape
    width = out_grad.shape[1]
    rows = down_weight.shape[0]
    nrep = lax.axis_size("rep")
    cols = ff // NP
    scale = 1.0 / math.sqrt(tok * nrep * lax.axis_size("fs"))
    dma = pltpu.SemaphoreType.DMA
    return pl.pallas_call(
        functools.partial(kernel, scale, nrep),
        out_shape=(
            jax.ShapeDtypeStruct((tok, ff), BF16),
            jax.ShapeDtypeStruct((rows, ff), F32),
        ),
        in_specs=[pl.BlockSpec(memory_space=pl.ANY)] * 3,
        out_specs=[pl.BlockSpec(memory_space=pltpu.VMEM)] * 2,
        scratch_shapes=[
            pltpu.VMEM((tok, ff), BF16),
            pltpu.VMEM((NK, tok, width // NK), BF16),
            pltpu.VMEM((NK, width // NK, tok), BF16),
            pltpu.VMEM((tok, ff), BF16),
            pltpu.VMEM((NP, NY, NK, rows, cols), BF16),
            pltpu.VMEM((NP, 2, NK // 2, rows, cols), BF16),
            pltpu.VMEM((NP, 2, NK // 2, rows, cols), BF16),
            pltpu.VMEM((NP, 2, NK, rows, cols), BF16),
            pltpu.VMEM((NP, NK, rows, cols), BF16),
            pltpu.VMEM((NP, NK - 1, rows, cols), BF16),
            pltpu.VMEM((NP, rows, cols), BF16),
            pltpu.VMEM((NP, nrep, rows // nrep, cols), BF16),
            pltpu.VMEM((NP, rows // nrep, cols), BF16),
            pltpu.VMEM((NP, nrep, rows // nrep, cols), BF16),
            pltpu.VMEM((NK, NY, rows, ff), BF16),
            pltpu.VMEM((tok, ff), F32),
            dma((NK + 2,)),
            dma((NP, 2)), dma((NP, 2)),
            dma((NP, 2)), dma((NP, 2)),
            dma((NP, 2)), dma((NP, 2)),
            dma((NP, 8)), dma((NP, 8)),
            dma((NP, nrep)), dma((NP, nrep)),
            dma((NP, nrep)), dma((NP, nrep)),
            dma((NK // 2, 2)), dma((NK // 2, 2)),
            dma((3, 2)), dma((3, 2)),
            pltpu.SemaphoreType.REGULAR((2,)),
        ],
        compiler_params=pltpu.CompilerParams(collective_id=0, has_side_effects=True),
    )(hidden_pre, out_grad, down_weight)


def solution(mesh):
    placed = (P(("rep", "fs"), "tp"), P(("rep", "fs"), None), P("fs", "tp"))
    return jax.shard_map(
        body,
        mesh=mesh,
        in_specs=placed,
        out_specs=(P(("rep", "fs"), "tp"), P("fs", "tp")),
        check_vma=False,
    )
```

```python
import functools
import math

import jax
import jax.numpy as jnp
from jax import lax
from jax.experimental import pallas as pl
from jax.experimental.pallas import tpu as pltpu
from jax.sharding import PartitionSpec as P

MESH = pl.DeviceIdType.MESH
NY = 4
NK = 8
NP = 4
ZOFF = (3, -3, 2, -2, 1, -1)
F32 = jnp.float32
BF16 = jnp.bfloat16


PASSES = ((0, 0, 64, 2), (1, 0, 64, 2), (2, 0, 64, 1), (3, 0, 32, 1), (3, 32, 32, 1))


def kernel(
    scale, nrep,
    hp_hbm, og_hbm, w_hbm, hg_hbm, wo_hbm,
    hp, og, ogt, ogp, act, part, arecv, bmerged, brecv, zsend, zrecv, qsend, qrecv, tsend, trecv, orecv, wall, back, hg, wo,
    lsem, osem, as_, ar_, us_, ur_, ms_, mr_, zs_, zr_, qs_, qr_, ts_, tr_, gzs, gzr, gys, gyr, near4,
):
    nz = nrep * NK
    h = lax.axis_index("rep")
    f = lax.axis_index("fs")
    k = f // NY
    j = lax.rem(f, NY)
    z = h * NK + k
    tok = hp.shape[0]
    rows = w_hbm.shape[0]
    cols = w_hbm.shape[1] // NP
    half = rows // 2
    j1, j2, j3 = lax.rem(j + 1, NY), lax.rem(j + 2, NY), lax.rem(j + 3, NY)

    def ydev(jj):
        return {"fs": k * NY + jj}

    def zdev(d):
        zz = lax.rem(z + d + nz, nz)
        return {"rep": zz // NK, "fs": lax.rem(zz, NK) * NY + j}

    def kk(d):
        return lax.rem(k + d + NK, NK)

    right, left = ydev(j1), ydev(j3)
    sends = []

    def send(src, dst, ss, rs, dev):
        c = pltpu.make_async_remote_copy(
            src_ref=src, dst_ref=dst, send_sem=ss, recv_sem=rs, device_id=dev, device_id_type=MESH
        )
        c.start()
        sends.append(c)

    def got(dst, rs):
        pltpu.make_async_remote_copy(
            src_ref=dst, dst_ref=dst, send_sem=rs, recv_sem=rs, device_id=right, device_id_type=MESH
        ).wait_recv()

    barrier = pltpu.get_barrier_semaphore()
    peers = [right, left] + [zdev(d) for d in (1, -1, 2, -2, 3, -3, 4, -4)]
    for peer in peers:
        pl.semaphore_signal(barrier, inc=1, device_id=peer, device_id_type=MESH)

    wide = NY * rows
    loads = []

    def load(src, dst, i):
        c = pltpu.make_async_copy(src, dst, lsem.at[i])
        c.start()
        loads.append(c)

    load(hp_hbm, hp, 0)
    for i in range(NK):
        load(og_hbm.at[:, pl.ds(i * wide, wide)], og.at[i], 1 + i)
    load(w_hbm, wall.at[j, k], 1 + NK)

    def load_act():
        loads[0].wait()
        pos = jnp.maximum(hp[...].astype(F32), 0.0)
        act[...] = (pos * pos).astype(BF16)

    def load_og():
        for i in range(NK):
            loads[1 + i].wait()
            t = og[i].T
            for jj in range(NY):
                ogt[jj, i * rows:(i + 1) * rows] = t[jj * rows:(jj + 1) * rows]

    def comp(c2, jj):
        res = jnp.dot(
            ogt[jj], act[:, 2 * c2 * cols:2 * (c2 + 1) * cols], preferred_element_type=F32
        ).astype(BF16)
        for c in range(2):
            part[2 * c2 + c, jj] = res[:, c * cols:(c + 1) * cols].reshape(NK, rows, cols)

    def comp_all(c2):
        @pl.loop(0, NY)
        def _(jj):
            comp(c2, jj)

    def near(i):
        if i > 0:
            pl.semaphore_wait(near4.at[i - 1], 2)
        for d in (4, -4):
            pl.semaphore_signal(near4.at[i], inc=1, device_id=zdev(d), device_id_type=MESH)

    lo, hi = pl.ds(0, NK // 2), pl.ds(NK // 2, NK // 2)

    def send_a(p):
        c, r0, nr, _ = PASSES[p]
        rr = pl.ds(r0, nr)
        send(part.at[c, j2, lo, rr], arecv.at[c, 0, :, rr], as_.at[p, 0], ar_.at[p, 0], right)
        send(part.at[c, j2, hi, rr], arecv.at[c, 1, :, rr], as_.at[p, 1], ar_.at[p, 1], left)

    def send_u(p):
        c, r0, nr, _ = PASSES[p]
        rr = pl.ds(r0, nr)
        send(part.at[c, j1, hi, rr], brecv.at[c, 0, hi, rr], us_.at[p, 0], ur_.at[p, 0], right)
        send(part.at[c, j3, lo, rr], brecv.at[c, 1, lo, rr], us_.at[p, 1], ur_.at[p, 1], left)

    def merge(p):
        c, r0, nr, _ = PASSES[p]
        rr = pl.ds(r0, nr)
        got(arecv.at[c, 0, :, rr], ar_.at[p, 0])
        bmerged[c, 0, :, rr] = (part[c, j1, lo, rr].astype(F32) + arecv[c, 0, :, rr].astype(F32)).astype(BF16)
        send(bmerged.at[c, 0, :, rr], brecv.at[c, 0, lo, rr], ms_.at[p, 0], mr_.at[p, 0], right)
        got(arecv.at[c, 1, :, rr], ar_.at[p, 1])
        bmerged[c, 1, :, rr] = (part[c, j3, hi, rr].astype(F32) + arecv[c, 1, :, rr].astype(F32)).astype(BF16)
        send(bmerged.at[c, 1, :, rr], brecv.at[c, 1, hi, rr], ms_.at[p, 1], mr_.at[p, 1], left)

    def ysum(c, i, rr):
        return (
            part[c, j, i, rr].astype(F32) + brecv[c, 0, i, rr].astype(F32) + brecv[c, 1, i, rr].astype(F32)
        )

    def recv_b(p):
        c, r0, nr, _ = PASSES[p]
        rr = pl.ds(r0, nr)
        got(brecv.at[c, 0, hi, rr], ur_.at[p, 0])
        got(brecv.at[c, 1, lo, rr], ur_.at[p, 1])
        got(brecv.at[c, 0, lo, rr], mr_.at[p, 0])
        got(brecv.at[c, 1, hi, rr], mr_.at[p, 1])
        zsend[c, :, rr] = ysum(c, slice(None), rr).astype(BF16)
        far = kk(4)
        up, dn = pl.ds(r0, nr // 2), pl.ds(r0 + nr // 2, nr // 2)
        send(zsend.at[c, far, dn], zrecv.at[c, 6, dn], zs_.at[p, 6], zr_.at[p, 6], zdev(4))
        send(zsend.at[c, far, up], zrecv.at[c, 6, up], zs_.at[p, 7], zr_.at[p, 7], zdev(-4))
        for s, d in enumerate(ZOFF):
            send(zsend.at[c, kk(d), rr], zrecv.at[c, s, rr], zs_.at[p, s], zr_.at[p, s], zdev(d))

    def recv_z(p):
        c, r0, nr, mode = PASSES[p]
        rr = pl.ds(r0, nr)
        up, dn = pl.ds(r0, nr // 2), pl.ds(r0 + nr // 2, nr // 2)
        got(zrecv.at[c, 6, dn], zr_.at[p, 6])
        got(zrecv.at[c, 6, up], zr_.at[p, 7])
        for s in range(len(ZOFF)):
            got(zrecv.at[c, s, rr], zr_.at[p, s])
        q = ysum(c, k, rr)
        for s in range(len(ZOFF) + 1):
            q = q + zrecv[c, s, rr].astype(F32)
        if mode == 2:
            quarter = nr // nrep
            qsend[c] = q.astype(BF16)
            for r in range(nrep):
                send(
                    qsend.at[c, pl.ds(r * quarter, quarter)], qrecv.at[c, h], qs_.at[p, r], qr_.at[p, h],
                    {"rep": r, "fs": kk(4) * NY + j},
                )
        else:
            orecv[c, h, rr] = q.astype(BF16)
            for i in (2, 1, 3):
                send(
                    orecv.at[c, h, rr], orecv.at[c, h, rr], qs_.at[p, i], qr_.at[p, i],
                    {"rep": lax.rem(h + i, nrep)},
                )

    def recv_q(p):
        c = PASSES[p][0]
        for r in range(nrep):
            got(qrecv.at[c, r], qr_.at[p, r])
        t = qrecv[c, 0].astype(F32)
        for r in range(1, nrep):
            t = t + qrecv[c, r].astype(F32)
        tsend[c] = (t * scale).astype(BF16)
        for r in range(nrep):
            send(tsend.at[c], trecv.at[c, h], ts_.at[p, r], tr_.at[p, h], {"rep": r, "fs": kk(4) * NY + j})

    def recv_t(p):
        c, r0, nr, mode = PASSES[p]
        cc = slice(c * cols, (c + 1) * cols)
        if mode == 2:
            quarter = nr // nrep
            for r in range(nrep):
                got(trecv.at[c, r], tr_.at[p, r])
                wo[r * quarter:(r + 1) * quarter, cc] = trecv[c, r].astype(F32)
        else:
            rr = pl.ds(r0, nr)
            for i in (2, 1, 3):
                got(orecv.at[c, lax.rem(h - i + nrep, nrep), rr], qr_.at[p, i])
            t = orecv[c, 0, rr].astype(F32)
            for r in range(1, nrep):
                t = t + orecv[c, r, rr].astype(F32)
            wo[rr, cc] = t * scale

    def gz(s):
        lower, upper = kk(-s), kk(s)
        if s == 0:
            loads[1 + NK].wait()
        if s > 0:
            got(wall.at[j, lower], gzr.at[s - 1, 0])
            got(wall.at[j, upper], gzr.at[s - 1, 1])
        if s < NK // 2 - 1:
            send(wall.at[j, lower], wall.at[j, lower], gzs.at[s, 0], gzr.at[s, 0], zdev(1))
            send(wall.at[j, upper], wall.at[j, upper], gzs.at[s, 1], gzr.at[s, 1], zdev(-1))
        else:
            a = wall.at[j, lower, pl.ds(0, half)]
            b = wall.at[j, upper, pl.ds(half, half)]
            send(a, a, gzs.at[s, 0], gzr.at[s, 0], zdev(1))
            send(b, b, gzs.at[s, 1], gzr.at[s, 1], zdev(-1))

    def gy_own():
        far = kk(4)
        got(wall.at[j, far, pl.ds(0, half)], gzr.at[NK // 2 - 1, 0])
        got(wall.at[j, far, pl.ds(half, half)], gzr.at[NK // 2 - 1, 1])
        a, b = wall.at[j, lo], wall.at[j, hi]
        send(a, a, gys.at[0, 0], gyr.at[0, 0], right)
        send(b, b, gys.at[0, 1], gyr.at[0, 1], left)
        send(b, b, gys.at[1, 0], gyr.at[1, 0], right)
        send(a, a, gys.at[1, 1], gyr.at[1, 1], left)

    def gy_forward():
        a, b = wall.at[j3, lo], wall.at[j1, hi]
        got(a, gyr.at[0, 0])
        send(a, a, gys.at[2, 0], gyr.at[2, 0], right)
        got(b, gyr.at[0, 1])
        send(b, b, gys.at[2, 1], gyr.at[2, 1], left)

    def gy_near():
        got(wall.at[j3, hi], gyr.at[1, 0])
        got(wall.at[j1, lo], gyr.at[1, 1])

    def gy_far():
        got(wall.at[j2, lo], gyr.at[2, 0])
        got(wall.at[j2, hi], gyr.at[2, 1])

    def w_block(jj):
        return jnp.dot(ogp[jj], wall[jj].reshape(NK * rows, wall.shape[-1]), preferred_element_type=F32)

    def w_own():
        @pl.loop(0, NY)
        def _(jj):
            ogp[jj] = ogt[jj].T

        back[...] = w_block(j)

    def w_near():
        back[...] += w_block(j3)
        back[...] += w_block(j1)

    def w_far():
        hg[...] = (2.0 * jnp.maximum(hp[...].astype(F32), 0.0) * (back[...] + w_block(j2))).astype(BF16)
        c = pltpu.make_async_copy(hg, hg_hbm, osem.at[0])
        c.start()
        loads.append(c)

    load_act()
    load_og()
    comp(0, j2)
    pl.semaphore_wait(barrier, len(peers))
    send_a(0)
    comp(0, j1)
    comp(0, j3)
    send_u(0)
    send_a(1)
    near(0)
    gz(0)
    comp(0, j)
    comp_all(1)
    merge(0)
    send_u(1)
    send_a(2)
    gz(1)
    near(1)
    merge(1)
    send_u(2)
    send_a(3)
    recv_b(0)
    gz(2)
    near(2)
    merge(2)
    send_u(3)
    send_a(4)
    recv_b(1)
    gz(3)
    pl.semaphore_wait(near4.at[2], 2)
    recv_z(0)
    merge(3)
    send_u(4)
    recv_b(2)
    merge(4)
    gy_own()
    recv_z(1)
    recv_b(3)
    recv_b(4)
    recv_z(2)
    recv_z(3)
    recv_q(0)
    recv_z(4)
    w_own()
    gy_forward()
    recv_q(1)
    gy_near()
    w_near()
    recv_t(0)
    recv_t(2)
    gy_far()
    w_far()
    recv_t(1)
    recv_t(3)
    recv_t(4)
    c = pltpu.make_async_copy(wo, wo_hbm, osem.at[1])
    c.start()
    loads[2 + NK].wait()
    c.wait()
    for c in sends:
        c.wait_send()


def body(hidden_pre, out_grad, down_weight):
    tok, ff = hidden_pre.shape
    width = out_grad.shape[1]
    rows = down_weight.shape[0]
    nrep = lax.axis_size("rep")
    cols = ff // NP
    npass = len(PASSES)
    scale = 1.0 / math.sqrt(tok * nrep * lax.axis_size("fs"))
    dma = pltpu.SemaphoreType.DMA
    return pl.pallas_call(
        functools.partial(kernel, scale, nrep),
        out_shape=(
            jax.ShapeDtypeStruct((tok, ff), BF16),
            jax.ShapeDtypeStruct((rows, ff), F32),
        ),
        in_specs=[pl.BlockSpec(memory_space=pl.ANY)] * 3,
        out_specs=[pl.BlockSpec(memory_space=pl.ANY)] * 2,
        scratch_shapes=[
            pltpu.VMEM((tok, ff), BF16),
            pltpu.VMEM((NK, tok, width // NK), BF16),
            pltpu.VMEM((NY, width // NY, tok), BF16),
            pltpu.VMEM((NY, tok, width // NY), BF16),
            pltpu.VMEM((tok, ff), BF16),
            pltpu.VMEM((NP, NY, NK, rows, cols), BF16),
            pltpu.VMEM((NP, 2, NK // 2, rows, cols), BF16),
            pltpu.VMEM((NP, 2, NK // 2, rows, cols), BF16),
            pltpu.VMEM((NP, 2, NK, rows, cols), BF16),
            pltpu.VMEM((NP, NK, rows, cols), BF16),
            pltpu.VMEM((NP, NK - 1, rows, cols), BF16),
            pltpu.VMEM((NP, rows, cols), BF16),
            pltpu.VMEM((NP, nrep, rows // nrep, cols), BF16),
            pltpu.VMEM((NP, rows // nrep, cols), BF16),
            pltpu.VMEM((NP, nrep, rows // nrep, cols), BF16),
            pltpu.VMEM((NP, nrep, rows, cols), BF16),
            pltpu.VMEM((NY, NK, rows, ff), BF16),
            pltpu.VMEM((tok, ff), F32),
            pltpu.VMEM((tok, ff), BF16),
            pltpu.VMEM((rows, ff), F32),
            dma((NK + 2,)),
            dma((2,)),
            dma((npass, 2)), dma((npass, 2)),
            dma((npass, 2)), dma((npass, 2)),
            dma((npass, 2)), dma((npass, 2)),
            dma((npass, 8)), dma((npass, 8)),
            dma((npass, nrep)), dma((npass, nrep)),
            dma((npass, nrep)), dma((npass, nrep)),
            dma((NK // 2, 2)), dma((NK // 2, 2)),
            dma((3, 2)), dma((3, 2)),
            pltpu.SemaphoreType.REGULAR((3,)),
        ],
        compiler_params=pltpu.CompilerParams(collective_id=0, has_side_effects=True),
    )(hidden_pre, out_grad, down_weight)


def solution(mesh):
    placed = (P(("rep", "fs"), "tp"), P(("rep", "fs"), None), P("fs", "tp"))
    return jax.shard_map(
        body,
        mesh=mesh,
        in_specs=placed,
        out_specs=(P(("rep", "fs"), "tp"), P("fs", "tp")),
        check_vma=False,
    )
```

```python
import functools
import math

import jax
import jax.numpy as jnp
from jax import lax
from jax.experimental import pallas as pl
from jax.experimental.pallas import tpu as pltpu
from jax.sharding import PartitionSpec as P

MESH = pl.DeviceIdType.MESH
NY = 4
NK = 8
NP = 4
VMEM_LIMIT = 32 * 1024 * 1024
F32 = jnp.float32
BF16 = jnp.bfloat16


PASSES = ((0, 0, 64, 2, 2), (1, 0, 64, 2, 2), (2, 0, 64, 1, 2), (3, 0, 32, 1, 1), (3, 32, 32, 1, 1))


def kernel(
    scale, nrep,
    hp_hbm, og_hbm, w_hbm, hg, wo,
    hp, og, ogt, ogp, act, part, arecv, bmerged, brecv, zsend, zpre, zrecv, zmerged, qsend, qrecv, tsend, trecv, orecv, wall, back,
    lsem, ys_, ar_, br_, zs_, zp_, zr_, qs_, qr_, ts_, tr_, gs, gzr, gyr, near4,
):
    nz = nrep * NK
    h = lax.axis_index("rep")
    f = lax.axis_index("fs")
    k = f // NY
    j = lax.rem(f, NY)
    z = h * NK + k
    tok = hp.shape[0]
    rows = w_hbm.shape[0]
    cols = w_hbm.shape[1] // NP
    half = rows // 2
    j1, j2, j3 = lax.rem(j + 1, NY), lax.rem(j + 2, NY), lax.rem(j + 3, NY)

    def ydev(jj):
        return {"fs": k * NY + jj}

    def zdev(d):
        zz = lax.rem(z + d + nz, nz)
        return {"rep": zz // NK, "fs": lax.rem(zz, NK) * NY + j}

    def kk(d):
        return lax.rem(k + d + NK, NK)

    right, left = ydev(j1), ydev(j3)

    def send(src, dst, ss, rs, dev):
        pltpu.make_async_remote_copy(
            src_ref=src, dst_ref=dst, send_sem=ss, recv_sem=rs, device_id=dev, device_id_type=MESH
        ).start()

    def got(dst, rs):
        pltpu.make_async_remote_copy(
            src_ref=dst, dst_ref=dst, send_sem=rs, recv_sem=rs, device_id=right, device_id_type=MESH
        ).wait_recv()

    def sent(src, ss):
        pltpu.make_async_remote_copy(
            src_ref=src, dst_ref=src, send_sem=ss, recv_sem=ss, device_id=right, device_id_type=MESH
        ).wait_send()

    barrier = pltpu.get_barrier_semaphore()
    peers = [right, left] + [zdev(d) for d in (1, -1, 2, -2, 3, -3, 4, -4)]
    for peer in peers:
        pl.semaphore_signal(barrier, inc=1, device_id=peer, device_id_type=MESH)

    wide = NY * rows
    loads = []

    def load(src, dst, i):
        c = pltpu.make_async_copy(src, dst, lsem.at[i])
        c.start()
        loads.append(c)

    load(hp_hbm, hp, 0)
    for i in range(NK):
        load(og_hbm.at[:, pl.ds(i * wide, wide)], og.at[i], 1 + i)
    load(w_hbm, wall.at[j, k], 1 + NK)

    def load_act():
        loads[0].wait()
        pos = jnp.maximum(hp[...].astype(F32), 0.0)
        act[...] = (pos * pos).astype(BF16)

    def load_og():
        for i in range(NK):
            loads[1 + i].wait()
            t = og[i].T
            for jj in range(NY):
                ogt[jj, i * rows:(i + 1) * rows] = t[jj * rows:(jj + 1) * rows]

    def comp(c2, jj):
        res = jnp.dot(
            ogt[jj], act[:, 2 * c2 * cols:2 * (c2 + 1) * cols], preferred_element_type=F32
        ).astype(BF16)
        for c in range(2):
            part[2 * c2 + c, jj] = res[:, c * cols:(c + 1) * cols].reshape(NK, rows, cols)

    def comp_all(c2):
        @pl.loop(0, NY)
        def _(jj):
            comp(c2, jj)

    def near(i):
        if i > 0:
            pl.semaphore_wait(near4.at[i - 1], 2)
        for d in (4, -4):
            pl.semaphore_signal(near4.at[i], inc=1, device_id=zdev(d), device_id_type=MESH)

    lo, hi = pl.ds(0, NK // 2), pl.ds(NK // 2, NK // 2)

    def send_a(p):
        c, r0, nr = PASSES[p][:3]
        rr = pl.ds(r0, nr)
        send(part.at[c, j2, lo, rr], arecv.at[c, 0, :, rr], ys_.at[p], ar_.at[p, 0], right)
        send(part.at[c, j2, hi, rr], arecv.at[c, 1, :, rr], ys_.at[p], ar_.at[p, 1], left)

    def send_u(p):
        c, r0, nr = PASSES[p][:3]
        rr = pl.ds(r0, nr)
        send(part.at[c, j1, hi, rr], brecv.at[c, 0, hi, rr], ys_.at[p], br_.at[p], right)
        send(part.at[c, j3, lo, rr], brecv.at[c, 1, lo, rr], ys_.at[p], br_.at[p], left)

    def merge(p):
        c, r0, nr = PASSES[p][:3]
        rr = pl.ds(r0, nr)
        got(arecv.at[c, 0, :, rr], ar_.at[p, 0])
        bmerged[c, 0, :, rr] = (part[c, j1, lo, rr].astype(F32) + arecv[c, 0, :, rr].astype(F32)).astype(BF16)
        send(bmerged.at[c, 0, :, rr], brecv.at[c, 0, lo, rr], ys_.at[p], br_.at[p], right)
        got(arecv.at[c, 1, :, rr], ar_.at[p, 1])
        bmerged[c, 1, :, rr] = (part[c, j3, hi, rr].astype(F32) + arecv[c, 1, :, rr].astype(F32)).astype(BF16)
        send(bmerged.at[c, 1, :, rr], brecv.at[c, 1, hi, rr], ys_.at[p], br_.at[p], left)

    def ysum(c, i, rr):
        return (
            part[c, j, i, rr].astype(F32) + brecv[c, 0, i, rr].astype(F32) + brecv[c, 1, i, rr].astype(F32)
        )

    def recv_b(p):
        c, r0, nr = PASSES[p][:3]
        rr = pl.ds(r0, nr)
        got(brecv.at[c, :, :, rr], br_.at[p])
        zsend[c, :, rr] = ysum(c, slice(None), rr).astype(BF16)
        far = kk(4)
        up, dn = pl.ds(r0, nr // 2), pl.ds(r0 + nr // 2, nr // 2)
        if PASSES[p][4] == 1:
            send(zsend.at[c, far, dn], zrecv.at[c, 6, dn], zs_.at[p], zr_.at[p], zdev(4))
            send(zsend.at[c, far, up], zrecv.at[c, 6, up], zs_.at[p], zr_.at[p], zdev(-4))
            for i, d in enumerate((3, -3, 2, -2, 1, -1)):
                send(zsend.at[c, kk(d), rr], zrecv.at[c, i, rr], zs_.at[p], zr_.at[p], zdev(d))
            return
        for i, d in enumerate((1, -1)):
            hh = (dn, up)[i]
            send(zsend.at[c, kk(3 * d), rr], zpre.at[c, i, 0, rr], zs_.at[p], zp_.at[p, i], zdev(d))
            send(zsend.at[c, far, hh], zpre.at[c, i, 1, pl.ds(0, nr // 2)], zs_.at[p], zp_.at[p, 2 + i], zdev(2 * d))
        for i, d in enumerate((1, -1)):
            send(zsend.at[c, kk(d), rr], zrecv.at[c, i, rr], zs_.at[p], zr_.at[p], zdev(d))

    def merge_z(p):
        c, r0, nr = PASSES[p][:3]
        rr = pl.ds(r0, nr)
        up, dn = pl.ds(r0, nr // 2), pl.ds(r0 + nr // 2, nr // 2)
        for i, d in enumerate((1, -1)):
            got(zpre.at[c, i, 0, rr], zp_.at[p, i])
            m = ysum(c, kk(2 * d), rr) + zpre[c, i, 0, rr].astype(F32)
            got(zpre.at[c, i, 1, pl.ds(0, nr // 2)], zp_.at[p, 2 + i])
            zero = jnp.zeros((nr // 2, cols), F32)
            add = zpre[c, i, 1, pl.ds(0, nr // 2)].astype(F32)
            m = m + jnp.concatenate(((zero, add), (add, zero))[i], axis=0)
            zmerged[c, i, rr] = m.astype(BF16)
            send(zmerged.at[c, i, rr], zrecv.at[c, 2 + i, rr], zs_.at[p], zr_.at[p], zdev(2 * d))

    def recv_z(p):
        c, r0, nr, mode, _ = PASSES[p]
        rr = pl.ds(r0, nr)
        q = ysum(c, k, rr)
        many = (7, 4)[PASSES[p][4] - 1]
        got(zrecv.at[c, pl.ds(0, many), rr], zr_.at[p])
        for i in range(many):
            q = q + zrecv[c, i, rr].astype(F32)
        if mode == 2:
            quarter = nr // nrep
            qsend[c] = q.astype(BF16)
            for r in range(nrep):
                send(
                    qsend.at[c, pl.ds(r * quarter, quarter)], qrecv.at[c, h], qs_.at[p], qr_.at[p],
                    {"rep": r, "fs": kk(4) * NY + j},
                )
        else:
            orecv[c, h, rr] = q.astype(BF16)
            for i in (2, 1, 3):
                send(
                    orecv.at[c, h, rr], orecv.at[c, h, rr], qs_.at[p], qr_.at[p],
                    {"rep": lax.rem(h + i, nrep)},
                )

    def recv_q(p):
        c = PASSES[p][0]
        got(qrecv.at[c], qr_.at[p])
        t = qrecv[c, 0].astype(F32)
        for r in range(1, nrep):
            t = t + qrecv[c, r].astype(F32)
        tsend[c] = (t * scale).astype(BF16)
        for r in range(nrep):
            send(tsend.at[c], trecv.at[c, h], ts_.at[p], tr_.at[p], {"rep": r, "fs": kk(4) * NY + j})

    def recv_t(p):
        c, r0, nr, mode, _ = PASSES[p]
        cc = slice(c * cols, (c + 1) * cols)
        if mode == 2:
            quarter = nr // nrep
            got(trecv.at[c], tr_.at[p])
            for r in range(nrep):
                wo[r * quarter:(r + 1) * quarter, cc] = trecv[c, r].astype(F32)
        else:
            rr = pl.ds(r0, nr)
            got(orecv.at[c, pl.ds(0, nrep - 1), rr], qr_.at[p])
            t = orecv[c, 0, rr].astype(F32)
            for r in range(1, nrep):
                t = t + orecv[c, r, rr].astype(F32)
            wo[rr, cc] = t * scale

    def gz(s):
        lower, upper = kk(-s), kk(s)
        if s == 0:
            loads[1 + NK].wait()
        if s > 0:
            got(wall.at[j, lower], gzr.at[s - 1, 0])
            got(wall.at[j, upper], gzr.at[s - 1, 1])
        if s < NK // 2 - 1:
            send(wall.at[j, lower], wall.at[j, lower], gs.at[0], gzr.at[s, 0], zdev(1))
            send(wall.at[j, upper], wall.at[j, upper], gs.at[0], gzr.at[s, 1], zdev(-1))
        else:
            a = wall.at[j, lower, pl.ds(0, half)]
            b = wall.at[j, upper, pl.ds(half, half)]
            send(a, a, gs.at[0], gzr.at[s, 0], zdev(1))
            send(b, b, gs.at[0], gzr.at[s, 1], zdev(-1))

    def gy_own():
        far = kk(4)
        got(wall.at[j, far, pl.ds(0, half)], gzr.at[NK // 2 - 1, 0])
        got(wall.at[j, far, pl.ds(half, half)], gzr.at[NK // 2 - 1, 1])
        a, b = wall.at[j, lo], wall.at[j, hi]
        send(a, a, gs.at[1], gyr.at[0], right)
        send(b, b, gs.at[1], gyr.at[1], left)
        send(b, b, gs.at[1], gyr.at[2], right)
        send(a, a, gs.at[1], gyr.at[2], left)

    def gy_forward():
        a, b = wall.at[j3, lo], wall.at[j1, hi]
        got(a, gyr.at[0])
        send(a, a, gs.at[1], gyr.at[3], right)
        got(b, gyr.at[1])
        send(b, b, gs.at[1], gyr.at[3], left)

    def gy_near():
        got(wall.at[j], gyr.at[2])

    def gy_far():
        got(wall.at[j2], gyr.at[3])

    def w_block(jj):
        return jnp.dot(ogp[jj], wall[jj].reshape(NK * rows, wall.shape[-1]), preferred_element_type=F32)

    def w_own():
        @pl.loop(0, NY)
        def _(jj):
            ogp[jj] = ogt[jj].T

        back[...] = w_block(j)

    def w_near():
        back[...] += w_block(j3)
        back[...] += w_block(j1)

    def w_far():
        hg[...] = (2.0 * jnp.maximum(hp[...].astype(F32), 0.0) * (back[...] + w_block(j2))).astype(BF16)

    def st_sends():
        for p, (c, r0, nr, mode, _) in enumerate(PASSES):
            rr = pl.ds(r0, nr)
            sent(part.at[c, pl.ds(0, 3), :, rr], ys_.at[p])
            sent(zsend.at[c, pl.ds(0, NK - 1), rr], zs_.at[p])
            if mode == 2:
                sent(qsend.at[c], qs_.at[p])
                sent(trecv.at[c], ts_.at[p])
            else:
                sent(orecv.at[c, pl.ds(0, nrep - 1), rr], qs_.at[p])
        sent(wall.at[j, pl.ds(0, NK - 1)], gs.at[0])
        sent(wall.at[pl.ds(0, 3)], gs.at[1])

    load_act()
    load_og()
    comp(0, j2)
    pl.semaphore_wait(barrier, len(peers))
    send_a(0)
    comp(0, j1)
    comp(0, j3)
    send_u(0)
    send_a(1)
    near(0)
    gz(0)
    comp(0, j)
    comp_all(1)
    merge(0)
    send_u(1)
    send_a(2)
    gz(1)
    near(1)
    merge(1)
    send_u(2)
    send_a(3)
    recv_b(0)
    gz(2)
    near(2)
    merge(2)
    send_u(3)
    send_a(4)
    recv_b(1)
    merge_z(0)
    gz(3)
    pl.semaphore_wait(near4.at[2], 2)
    merge(3)
    send_u(4)
    recv_z(0)
    recv_b(2)
    merge_z(1)
    merge(4)
    gy_own()
    recv_b(3)
    recv_z(1)
    merge_z(2)
    recv_b(4)
    recv_z(3)
    recv_z(2)
    recv_z(4)
    recv_q(0)
    w_own()
    gy_forward()
    recv_q(1)
    gy_near()
    w_near()
    recv_t(0)
    recv_t(2)
    gy_far()
    w_far()
    recv_t(3)
    recv_t(4)
    recv_t(1)
    st_sends()


def body(hidden_pre, out_grad, down_weight):
    tok, ff = hidden_pre.shape
    width = out_grad.shape[1]
    rows = down_weight.shape[0]
    nrep = lax.axis_size("rep")
    cols = ff // NP
    npass = len(PASSES)
    scale = 1.0 / math.sqrt(tok * nrep * lax.axis_size("fs"))
    dma = pltpu.SemaphoreType.DMA
    hg, wo = pl.pallas_call(
        functools.partial(kernel, scale, nrep),
        out_shape=(pltpu.VMEM((tok, ff), BF16), pltpu.VMEM((rows, ff), F32)),
        in_specs=[pl.BlockSpec(memory_space=pltpu.HBM)] * 3,
        out_specs=[pl.BlockSpec(memory_space=pltpu.VMEM)] * 2,
        scratch_shapes=[
            pltpu.VMEM((tok, ff), BF16),
            pltpu.VMEM((NK, tok, width // NK), BF16),
            pltpu.VMEM((NY, width // NY, tok), BF16),
            pltpu.VMEM((NY, tok, width // NY), BF16),
            pltpu.VMEM((tok, ff), BF16),
            pltpu.VMEM((NP, NY, NK, rows, cols), BF16),
            pltpu.VMEM((NP, 2, NK // 2, rows, cols), BF16),
            pltpu.VMEM((NP, 2, NK // 2, rows, cols), BF16),
            pltpu.VMEM((NP, 2, NK, rows, cols), BF16),
            pltpu.VMEM((NP, NK, rows, cols), BF16),
            pltpu.VMEM((NP, 2, 2, rows, cols), BF16),
            pltpu.VMEM((NP, NK - 1, rows, cols), BF16),
            pltpu.VMEM((NP, 2, rows, cols), BF16),
            pltpu.VMEM((NP, rows, cols), BF16),
            pltpu.VMEM((NP, nrep, rows // nrep, cols), BF16),
            pltpu.VMEM((NP, rows // nrep, cols), BF16),
            pltpu.VMEM((NP, nrep, rows // nrep, cols), BF16),
            pltpu.VMEM((NP, nrep, rows, cols), BF16),
            pltpu.VMEM((NY, NK, rows, ff), BF16),
            pltpu.VMEM((tok, ff), F32),
            dma((NK + 2,)),
            dma((npass,)), dma((npass, 2)), dma((npass,)),
            dma((npass,)), dma((npass, 4)), dma((npass,)),
            dma((npass,)), dma((npass,)), dma((npass,)), dma((npass,)),
            dma((2,)), dma((NK // 2, 2)), dma((4,)),
            pltpu.SemaphoreType.REGULAR((3,)),
        ],
        compiler_params=pltpu.CompilerParams(collective_id=0, has_side_effects=True, vmem_limit_bytes=VMEM_LIMIT),
    )(*(pltpu.with_memory_space_constraint(x, pltpu.HBM) for x in (hidden_pre, out_grad, down_weight)))
    return hg, wo


def solution(mesh):
    placed = (P(("rep", "fs"), "tp"), P(("rep", "fs"), None), P("fs", "tp"))
    return jax.shard_map(
        body,
        mesh=mesh,
        in_specs=placed,
        out_specs=(P(("rep", "fs"), "tp"), P("fs", "tp")),
        check_vma=False,
    )
```

```python
import functools
import math

import jax
import jax.numpy as jnp
from jax import lax
from jax.experimental import pallas as pl
from jax.experimental.pallas import tpu as pltpu
from jax.sharding import PartitionSpec as P

MESH = pl.DeviceIdType.MESH
NY = 4
NK = 8
NP = 4
VMEM_LIMIT = 32 * 1024 * 1024
F32 = jnp.float32
BF16 = jnp.bfloat16


PASSES = ((0, 0, 64, 2), (1, 0, 64, 2), (2, 0, 64, 2), (3, 0, 32, 1), (3, 32, 32, 1))


def kernel(
    scale, nrep,
    hp_hbm, og_hbm, w_hbm, hg, wo,
    hp, og, ogt, ogp, act, part, arecv, bmerged, brecv, zsend, zpre, zrecv, zmerged, xq, xr, xt, xu, wall, back,
    lsem, ys_, ar_, br_, zs_, zp_, zr_, xs_, xr_, xu_, gs, gzr, gyr, near4,
):
    nz = nrep * NK
    h = lax.axis_index("rep")
    f = lax.axis_index("fs")
    k = f // NY
    j = lax.rem(f, NY)
    z = h * NK + k
    tok = hp.shape[0]
    rows = w_hbm.shape[0]
    cols = w_hbm.shape[1] // NP
    half = rows // 2
    j1, j2, j3 = lax.rem(j + 1, NY), lax.rem(j + 2, NY), lax.rem(j + 3, NY)

    def ydev(jj):
        return {"fs": k * NY + jj}

    def zdev(d):
        zz = lax.rem(z + d + nz, nz)
        return {"rep": zz // NK, "fs": lax.rem(zz, NK) * NY + j}

    def kk(d):
        return lax.rem(k + d + NK, NK)

    right, left = ydev(j1), ydev(j3)
    turn = 8 - 16 * lax.rem(h, 2)
    peer, other = zdev(turn), zdev(-turn)

    def send(src, dst, ss, rs, dev):
        pltpu.make_async_remote_copy(
            src_ref=src, dst_ref=dst, send_sem=ss, recv_sem=rs, device_id=dev, device_id_type=MESH
        ).start()

    def got(dst, rs):
        pltpu.make_async_remote_copy(
            src_ref=dst, dst_ref=dst, send_sem=rs, recv_sem=rs, device_id=right, device_id_type=MESH
        ).wait_recv()

    def sent(src, ss):
        pltpu.make_async_remote_copy(
            src_ref=src, dst_ref=src, send_sem=ss, recv_sem=ss, device_id=right, device_id_type=MESH
        ).wait_send()

    barrier = pltpu.get_barrier_semaphore()
    peers = [right, left] + [zdev(d) for d in (1, -1, 2, -2, 3, -3, 4, -4)]
    for dev in peers:
        pl.semaphore_signal(barrier, inc=1, device_id=dev, device_id_type=MESH)

    wide = NY * rows
    loads = []

    def load(src, dst, i):
        c = pltpu.make_async_copy(src, dst, lsem.at[i])
        c.start()
        loads.append(c)

    load(hp_hbm, hp, 0)
    for i in range(NK):
        load(og_hbm.at[:, pl.ds(i * wide, wide)], og.at[i], 1 + i)
    load(w_hbm, wall.at[j, k], 1 + NK)

    def load_act():
        loads[0].wait()
        pos = jnp.maximum(hp[...].astype(F32), 0.0)
        act[...] = (pos * pos).astype(BF16)

    def load_og():
        for i in range(NK):
            loads[1 + i].wait()
            t = og[i].T
            for jj in range(NY):
                ogt[jj, i * rows:(i + 1) * rows] = t[jj * rows:(jj + 1) * rows]

    def comp(c2, jj):
        res = jnp.dot(
            ogt[jj], act[:, 2 * c2 * cols:2 * (c2 + 1) * cols], preferred_element_type=F32
        ).astype(BF16)
        for c in range(2):
            part[2 * c2 + c, jj] = res[:, c * cols:(c + 1) * cols].reshape(NK, rows, cols)

    def comp_all(c2):
        @pl.loop(0, NY)
        def _(jj):
            comp(c2, jj)

    def near(i):
        if i > 0:
            pl.semaphore_wait(near4.at[i - 1], 2)
        for d in (4, -4):
            pl.semaphore_signal(near4.at[i], inc=1, device_id=zdev(d), device_id_type=MESH)

    lo, hi = pl.ds(0, NK // 2), pl.ds(NK // 2, NK // 2)

    def send_a(p):
        c, r0, nr = PASSES[p][:3]
        rr = pl.ds(r0, nr)
        send(part.at[c, j2, lo, rr], arecv.at[c, 0, :, rr], ys_.at[p], ar_.at[p, 0], right)
        send(part.at[c, j2, hi, rr], arecv.at[c, 1, :, rr], ys_.at[p], ar_.at[p, 1], left)

    def send_u(p):
        c, r0, nr = PASSES[p][:3]
        rr = pl.ds(r0, nr)
        send(part.at[c, j1, hi, rr], brecv.at[c, 0, hi, rr], ys_.at[p], br_.at[p], right)
        send(part.at[c, j3, lo, rr], brecv.at[c, 1, lo, rr], ys_.at[p], br_.at[p], left)

    def merge(p):
        c, r0, nr = PASSES[p][:3]
        rr = pl.ds(r0, nr)
        got(arecv.at[c, 0, :, rr], ar_.at[p, 0])
        bmerged[c, 0, :, rr] = (part[c, j1, lo, rr].astype(F32) + arecv[c, 0, :, rr].astype(F32)).astype(BF16)
        send(bmerged.at[c, 0, :, rr], brecv.at[c, 0, lo, rr], ys_.at[p], br_.at[p], right)
        got(arecv.at[c, 1, :, rr], ar_.at[p, 1])
        bmerged[c, 1, :, rr] = (part[c, j3, hi, rr].astype(F32) + arecv[c, 1, :, rr].astype(F32)).astype(BF16)
        send(bmerged.at[c, 1, :, rr], brecv.at[c, 1, hi, rr], ys_.at[p], br_.at[p], left)

    def ysum(c, i, rr):
        return (
            part[c, j, i, rr].astype(F32) + brecv[c, 0, i, rr].astype(F32) + brecv[c, 1, i, rr].astype(F32)
        )

    def recv_b(p):
        c, r0, nr = PASSES[p][:3]
        rr = pl.ds(r0, nr)
        got(brecv.at[c, :, :, rr], br_.at[p])
        zsend[c, :, rr] = ysum(c, slice(None), rr).astype(BF16)
        far = kk(4)
        up, dn = pl.ds(r0, nr // 2), pl.ds(r0 + nr // 2, nr // 2)
        if PASSES[p][3] == 1:
            send(zsend.at[c, far, dn], zrecv.at[c, 6, dn], zs_.at[p], zr_.at[p], zdev(4))
            send(zsend.at[c, far, up], zrecv.at[c, 6, up], zs_.at[p], zr_.at[p], zdev(-4))
            for i, d in enumerate((3, -3, 2, -2, 1, -1)):
                send(zsend.at[c, kk(d), rr], zrecv.at[c, i, rr], zs_.at[p], zr_.at[p], zdev(d))
            return
        for i, d in enumerate((1, -1)):
            hh = (dn, up)[i]
            send(zsend.at[c, kk(3 * d), rr], zpre.at[c, i, 0, rr], zs_.at[p], zp_.at[p, i], zdev(d))
            send(zsend.at[c, far, hh], zpre.at[c, i, 1, pl.ds(0, nr // 2)], zs_.at[p], zp_.at[p, 2 + i], zdev(2 * d))
        for i, d in enumerate((1, -1)):
            send(zsend.at[c, kk(d), rr], zrecv.at[c, i, rr], zs_.at[p], zr_.at[p], zdev(d))

    def merge_z(p):
        c, r0, nr = PASSES[p][:3]
        rr = pl.ds(r0, nr)
        up, dn = pl.ds(r0, nr // 2), pl.ds(r0 + nr // 2, nr // 2)
        for i, d in enumerate((1, -1)):
            got(zpre.at[c, i, 0, rr], zp_.at[p, i])
            m = ysum(c, kk(2 * d), rr) + zpre[c, i, 0, rr].astype(F32)
            got(zpre.at[c, i, 1, pl.ds(0, nr // 2)], zp_.at[p, 2 + i])
            zero = jnp.zeros((nr // 2, cols), F32)
            add = zpre[c, i, 1, pl.ds(0, nr // 2)].astype(F32)
            m = m + jnp.concatenate(((zero, add), (add, zero))[i], axis=0)
            zmerged[c, i, rr] = m.astype(BF16)
            send(zmerged.at[c, i, rr], zrecv.at[c, 2 + i, rr], zs_.at[p], zr_.at[p], zdev(2 * d))

    def recv_z(p):
        c, r0, nr = PASSES[p][:3]
        rr, up, dn = pl.ds(r0, nr), pl.ds(r0, nr // 2), pl.ds(r0 + nr // 2, nr // 2)
        q = ysum(c, k, rr)
        many = (7, 4)[PASSES[p][3] - 1]
        got(zrecv.at[c, pl.ds(0, many), rr], zr_.at[p])
        for i in range(many):
            q = q + zrecv[c, i, rr].astype(F32)
        xq[c, rr] = q.astype(BF16)
        send(xq.at[c, up], xr.at[c, up], xs_.at[p], xr_.at[p], peer)
        send(xq.at[c, dn], xr.at[c, dn], xs_.at[p], xr_.at[p], other)

    def recv_x(p):
        c, r0, nr = PASSES[p][:3]
        rr, up, dn = pl.ds(r0, nr), pl.ds(r0, nr // 2), pl.ds(r0 + nr // 2, nr // 2)
        got(xr.at[c, rr], xr_.at[p])
        xt[c, rr] = (xq[c, rr].astype(F32) + xr[c, rr].astype(F32)).astype(BF16)
        send(xt.at[c, up], xu.at[c, up], xs_.at[p], xu_.at[p], other)
        send(xt.at[c, dn], xu.at[c, dn], xs_.at[p], xu_.at[p], peer)

    def recv_t(p):
        c, r0, nr = PASSES[p][:3]
        rr = pl.ds(r0, nr)
        got(xu.at[c, rr], xu_.at[p])
        wo[rr, c * cols:(c + 1) * cols] = (xt[c, rr].astype(F32) + xu[c, rr].astype(F32)) * scale

    def gz(s):
        lower, upper = kk(-s), kk(s)
        if s == 0:
            loads[1 + NK].wait()
        if s > 0:
            got(wall.at[j, lower], gzr.at[s - 1, 0])
            got(wall.at[j, upper], gzr.at[s - 1, 1])
        if s < NK // 2 - 1:
            send(wall.at[j, lower], wall.at[j, lower], gs.at[0], gzr.at[s, 0], zdev(1))
            send(wall.at[j, upper], wall.at[j, upper], gs.at[0], gzr.at[s, 1], zdev(-1))
        else:
            a = wall.at[j, lower, pl.ds(0, half)]
            b = wall.at[j, upper, pl.ds(half, half)]
            send(a, a, gs.at[0], gzr.at[s, 0], zdev(1))
            send(b, b, gs.at[0], gzr.at[s, 1], zdev(-1))

    def gy_own():
        far = kk(4)
        got(wall.at[j, far, pl.ds(0, half)], gzr.at[NK // 2 - 1, 0])
        got(wall.at[j, far, pl.ds(half, half)], gzr.at[NK // 2 - 1, 1])
        a, b = wall.at[j, lo], wall.at[j, hi]
        send(a, a, gs.at[1], gyr.at[0], right)
        send(b, b, gs.at[1], gyr.at[1], left)
        send(b, b, gs.at[1], gyr.at[2], right)
        send(a, a, gs.at[1], gyr.at[2], left)

    def gy_forward():
        a, b = wall.at[j3, lo], wall.at[j1, hi]
        got(a, gyr.at[0])
        send(a, a, gs.at[1], gyr.at[3], right)
        got(b, gyr.at[1])
        send(b, b, gs.at[1], gyr.at[3], left)

    def gy_near():
        got(wall.at[j], gyr.at[2])

    def gy_far():
        got(wall.at[j2], gyr.at[3])

    def w_block(jj):
        return jnp.dot(ogp[jj], wall[jj].reshape(NK * rows, wall.shape[-1]), preferred_element_type=F32)

    def w_own():
        @pl.loop(0, NY)
        def _(jj):
            ogp[jj] = ogt[jj].T

        back[...] = w_block(j)

    def w_near():
        back[...] += w_block(j3)
        back[...] += w_block(j1)

    def w_far():
        hg[...] = (2.0 * jnp.maximum(hp[...].astype(F32), 0.0) * (back[...] + w_block(j2))).astype(BF16)

    def st_sends():
        for p, (c, r0, nr, _) in enumerate(PASSES):
            rr = pl.ds(r0, nr)
            sent(part.at[c, pl.ds(0, 3), :, rr], ys_.at[p])
            sent(zsend.at[c, pl.ds(0, NK - 1), rr], zs_.at[p])
            sent(zsend.at[c, pl.ds(0, 2), rr], xs_.at[p])
        sent(wall.at[j, pl.ds(0, NK - 1)], gs.at[0])
        sent(wall.at[pl.ds(0, 3)], gs.at[1])

    load_act()
    load_og()
    comp(0, j2)
    pl.semaphore_wait(barrier, len(peers))
    send_a(0)
    comp(0, j1)
    comp(0, j3)
    send_u(0)
    send_a(1)
    near(0)
    gz(0)
    comp(0, j)
    comp_all(1)
    merge(0)
    send_u(1)
    send_a(2)
    gz(1)
    merge(1)
    send_u(2)
    send_a(3)
    recv_b(0)
    gz(2)
    merge(2)
    send_u(3)
    send_a(4)
    recv_b(1)
    merge_z(0)
    gz(3)
    pl.semaphore_wait(near4.at[0], 2)
    merge(3)
    send_u(4)
    recv_z(0)
    recv_b(2)
    merge_z(1)
    merge(4)
    gy_own()
    recv_b(3)
    recv_z(1)
    merge_z(2)
    recv_b(4)
    recv_x(0)
    recv_z(3)
    recv_z(2)
    recv_z(4)
    gy_forward()
    recv_x(1)
    w_own()
    recv_x(3)
    recv_x(2)
    recv_x(4)
    gy_near()
    w_near()
    recv_t(0)
    recv_t(1)
    gy_far()
    w_far()
    recv_t(3)
    recv_t(2)
    recv_t(4)
    st_sends()


def body(hidden_pre, out_grad, down_weight):
    tok, ff = hidden_pre.shape
    width = out_grad.shape[1]
    rows = down_weight.shape[0]
    nrep = lax.axis_size("rep")
    cols = ff // NP
    npass = len(PASSES)
    scale = 1.0 / math.sqrt(tok * nrep * lax.axis_size("fs"))
    dma = pltpu.SemaphoreType.DMA
    hg, wo = pl.pallas_call(
        functools.partial(kernel, scale, nrep),
        out_shape=(pltpu.VMEM((tok, ff), BF16), pltpu.VMEM((rows, ff), F32)),
        in_specs=[pl.BlockSpec(memory_space=pltpu.HBM)] * 3,
        out_specs=[pl.BlockSpec(memory_space=pltpu.VMEM)] * 2,
        scratch_shapes=[
            pltpu.VMEM((tok, ff), BF16),
            pltpu.VMEM((NK, tok, width // NK), BF16),
            pltpu.VMEM((NY, width // NY, tok), BF16),
            pltpu.VMEM((NY, tok, width // NY), BF16),
            pltpu.VMEM((tok, ff), BF16),
            pltpu.VMEM((NP, NY, NK, rows, cols), BF16),
            pltpu.VMEM((NP, 2, NK // 2, rows, cols), BF16),
            pltpu.VMEM((NP, 2, NK // 2, rows, cols), BF16),
            pltpu.VMEM((NP, 2, NK, rows, cols), BF16),
            pltpu.VMEM((NP, NK, rows, cols), BF16),
            pltpu.VMEM((NP, 2, 2, rows, cols), BF16),
            pltpu.VMEM((NP, NK - 1, rows, cols), BF16),
            pltpu.VMEM((NP, 2, rows, cols), BF16),
            pltpu.VMEM((NP, rows, cols), BF16),
            pltpu.VMEM((NP, rows, cols), BF16),
            pltpu.VMEM((NP, rows, cols), BF16),
            pltpu.VMEM((NP, rows, cols), BF16),
            pltpu.VMEM((NY, NK, rows, ff), BF16),
            pltpu.VMEM((tok, ff), F32),
            dma((NK + 2,)),
            dma((npass,)), dma((npass, 2)), dma((npass,)),
            dma((npass,)), dma((npass, 4)), dma((npass,)),
            dma((npass,)), dma((npass,)), dma((npass,)),
            dma((2,)), dma((NK // 2, 2)), dma((4,)),
            pltpu.SemaphoreType.REGULAR((1,)),
        ],
        compiler_params=pltpu.CompilerParams(collective_id=0, has_side_effects=True, vmem_limit_bytes=VMEM_LIMIT),
    )(*(pltpu.with_memory_space_constraint(x, pltpu.HBM) for x in (hidden_pre, out_grad, down_weight)))
    return hg, wo


def solution(mesh):
    placed = (P(("rep", "fs"), "tp"), P(("rep", "fs"), None), P("fs", "tp"))
    return jax.shard_map(
        body,
        mesh=mesh,
        in_specs=placed,
        out_specs=(P(("rep", "fs"), "tp"), P("fs", "tp")),
        check_vma=False,
    )
```
